32 devices in a mesh: gr: 2 (over x), fs: 8 (over z, y), tp: 2 (over core).
Axes of the slice: x: 2, y: 2, z: 4, core: 2. Of those that a mesh axis runs over, the one named last changes fastest.
Arguments:
- tokens: bfloat16 [2816, 2048], P(('gr', 'fs')), may hold values from -6 to 6
- expert_ids: int32 [2816, 8], P(('gr', 'fs')), may hold values from 0 to 15, all different within a row; in each aligned block of 176 rows (0 to 175, 176 to 351, ...) at most 110 rows name the same one
- route_weight: float32 [2816, 8], P(('gr', 'fs')), may hold values from 0.05 to 1
- norm_gain: float32 [2048], P('tp'), may hold values from 0.1 to 1.9
- expert_gate: float32 [16, 512, 2048], P('gr', 'fs', 'tp'), may hold values from -0.125 to 0.125
- expert_up: float32 [16, 512, 2048], P('gr', 'fs', 'tp'), may hold values from -0.125 to 0.125
- expert_down: float32 [16, 512, 2048], P('gr', 'fs', 'tp'), may hold values from -0.25 to 0.25
- shared_gate: float32 [512, 2048], P('fs', 'tp'), may hold values from -0.125 to 0.125
- shared_up: float32 [512, 2048], P('fs', 'tp'), may hold values from -0.125 to 0.125
- shared_down: float32 [512, 2048], P('fs', 'tp'), may hold values from -0.25 to 0.25
Outputs:
- mixed: bfloat16 [2816, 2048], P(('gr', 'fs'), 'tp')
- new_gate: bfloat16 [2, 8, 512, 2048], P(None, 'fs', None, 'tp')
- new_up: bfloat16 [2, 8, 512, 2048], P(None, 'fs', None, 'tp')
- new_down: bfloat16 [2, 8, 512, 2048], P(None, 'fs', None, 'tp')
- new_shared_gate: bfloat16 [512, 2048], P(None, 'tp')
- new_shared_up: bfloat16 [512, 2048], P(None, 'tp')
- new_shared_down: bfloat16 [512, 2048], P(None, 'tp')
The draws below stay inside these ranges and needn't reach their ends.
Inputs may be any that keep to these rules, and one draw needn't show every extreme that they name: `expert_ids`: each row names 8 different experts; within each aligned block of 176 rows no expert is named by more than 110 rows, a bound that some block reaches.
All inputs are finite; a program needn't handle non-finite values.
Results may differ from the reference program's by a relative error of at most 0.022.
Values may be sent and summed in bfloat16 or wider, within the bound.
No kernel may reach another device: no remote copies, remote signals or barrier semaphores. Data moves between devices by JAX's collectives and lax.ppermute only.
A program may use at most 128 MiB of HBM per device.

```python
import math
import jax
import jax.numpy as jnp
import numpy as np
from jax import lax

D = 2048
FF = 512
SHARED = 512
TOP = 8
TOK_DEV = 176
EXPERTS = 16
CAP = 110
TOKENS = 2816
N_GR = 2
N_FS = 8
N_TP = 2


def shard_levels(key, extent, shards, low, high):
    factor_of, own = 1.0, jax.random.fold_in(key, 6)
    for position, shards_of in shards:
        heights = jnp.exp(jax.random.uniform(jax.random.fold_in(own, position), (shards_of,), jnp.float32, low / len(shards), high / len(shards)))
        factor_of = factor_of * jnp.repeat(heights, extent[position] // shards_of).reshape([-1 if axis == position else 1 for axis in range(len(extent))])
    return factor_of


def routed_block(stream_key, own, number, rows, amount, top, limit, slope):
    sequence = jax.random.permutation(stream_key, amount)
    crowded, common = shares(amount, rows * top, limit, slope, True), shares(amount, rows * top, limit, slope, False)
    places = jnp.arange(amount)

    def named(tallies, offset_by):
        used = int((tallies > 0).sum())
        fixed = max(1, used // 4)
        moved = fixed + (places - fixed + offset_by * (used - fixed)) % max(1, amount - fixed)
        return jnp.zeros((amount,), jnp.int32).at[sequence[jnp.where(places < fixed, places, moved)]].set(jnp.asarray(tallies, jnp.int32))

    tallies = jnp.where(number % 4 == 0, named(crowded, number // 4), named(common, number - number // 4 - 1))
    mixed = jax.random.permutation(jax.random.fold_in(own, 3), amount)
    giver, taker = mixed[0:amount // 2 * 2:2], mixed[1:amount // 2 * 2:2]
    slack = jnp.minimum(tallies[giver] - 1, limit - tallies[taker]) // 2
    slack = jnp.where((giver == sequence[0]) | (taker == sequence[0]) | (tallies[taker] == 0), 0, jnp.maximum(slack, 0))
    moved = jax.random.randint(jax.random.fold_in(own, 4), (amount // 2,), 0, 1 << 20) % (slack + 1)
    tallies = tallies.at[giver].add(-moved).at[taker].add(moved)
    labels = jnp.searchsorted(jnp.cumsum(tallies), jnp.arange(rows * top), side="right").astype(jnp.int32)
    listing = labels.reshape(top, rows).T
    listing = listing[jax.random.permutation(jax.random.fold_in(own, 1), rows)]
    offset_by = jax.random.randint(jax.random.fold_in(own, 2), (rows, 1), 0, top)
    return jnp.take_along_axis(listing, (jnp.arange(top)[None, :] + offset_by) % top, axis=1)


def shares(count, total, bound, slope, full):
    loads = [(1 << 20) // math.isqrt(grade ** slope) + 1 for grade in range(1, count + 1)]
    largest = bound if full else min(bound, max(-(-total // count), total * loads[0] // sum(loads)))
    least = 1 if total - largest >= count - 1 else 0
    counts, surplus = [largest] + [least] * (count - 1), total - largest - least * (count - 1)
    while surplus > 0:
        candidates = [i for i in range(1, count) if counts[i] < largest] or [i for i in range(1, count) if counts[i] < bound]
        whole, left = sum([loads[i] for i in candidates]), surplus
        for i in candidates:
            more = min(bound - counts[i], max(1, left * loads[i] // whole), surplus)
            counts[i] = counts[i] + more
            surplus = surplus - more
    return np.array(counts)


def centred(own_key, dims, spread, reach, pieces=(), kind=jnp.bfloat16):
    entries = spread * jax.random.normal(own_key, dims, jnp.float32)
    if pieces:
        entries = entries * shard_levels(own_key, dims, pieces, -0.22, 0.18)
    return jnp.clip(entries, -reach, reach).astype(kind)


def setup_inputs(seed: int = 0) -> dict:
    splits = jax.random.split(jax.random.key(seed), 11)
    tokens = centred(splits[0], (TOKENS, D), 1.0, 6.0, ((0, 16),))
    expert_ids_keys = jax.random.split(jax.random.fold_in(splits[1], 1), TOKENS // TOK_DEV)
    expert_ids_turns = jax.random.permutation(jax.random.fold_in(splits[1], 3), TOKENS // TOK_DEV)
    expert_ids = jax.vmap(lambda own, number: routed_block(jax.random.fold_in(splits[1], 2), own, number, TOK_DEV, EXPERTS, TOP, CAP, 1))(expert_ids_keys, expert_ids_turns).reshape((TOKENS, TOP))
    route_weight = jnp.clip(jnp.exp(math.log(1.0) - 2.9957323 * jax.random.uniform(splits[2], (TOKENS, TOP), jnp.float32) ** shard_levels(splits[2], (TOKENS, TOP), ((0, 16),), -0.2, 0.2)), 0.05, 1.0)
    norm_gain = jnp.clip(1.0 + 0.18 * jax.random.normal(splits[3], (D,), jnp.float32), 0.1, 1.9)
    expert_gate = centred(splits[4], (EXPERTS, FF, D), D ** -0.5, 0.125, ((0, 2), (1, 8), (2, 2)), jnp.float32)
    expert_up = centred(splits[5], (EXPERTS, FF, D), D ** -0.5, 0.125, ((0, 2), (1, 8), (2, 2)), jnp.float32)
    expert_down = centred(splits[6], (EXPERTS, FF, D), FF ** -0.5, 0.25, ((0, 2), (1, 8), (2, 2)), jnp.float32)
    shared_gate = centred(splits[7], (SHARED, D), D ** -0.5, 0.125, ((0, 8), (1, 2)), jnp.float32)
    shared_up = centred(splits[8], (SHARED, D), D ** -0.5, 0.125, ((0, 8), (1, 2)), jnp.float32)
    shared_down = centred(splits[9], (SHARED, D), SHARED ** -0.5, 0.25, ((0, 8), (1, 2)), jnp.float32)
    return dict(tokens=tokens, expert_ids=expert_ids, route_weight=route_weight, norm_gain=norm_gain, expert_gate=expert_gate, expert_up=expert_up, expert_down=expert_down, shared_gate=shared_gate, shared_up=shared_up, shared_down=shared_down)


route_scale = 2.5
norm_eps = 1e-06

def blocked_product(rows, weight):
    count = rows.shape[0]
    left = rows.astype(jnp.float32).reshape(count, N_TP, D // N_TP)
    right = weight.astype(jnp.float32).reshape(weight.shape[0], N_TP, D // N_TP)
    parts = jnp.einsum('mbd,fbd->bmf', left, right, precision=lax.Precision.HIGHEST).astype(jnp.bfloat16)
    parts = lax.optimization_barrier(parts)
    return lax.optimization_barrier(jnp.sum(parts.astype(jnp.float32), axis=0))

def feed_forward(rows, gate_weight, up_weight):
    gate_pre = blocked_product(rows, gate_weight)
    up_pre = blocked_product(rows, up_weight)
    return (jax.nn.silu(gate_pre) * up_pre).astype(jnp.bfloat16)

def reference(tokens, expert_ids, route_weight, norm_gain, expert_gate, expert_up, expert_down, shared_gate, shared_up, shared_down):
    gate_round = (expert_gate * norm_gain).astype(jnp.bfloat16)
    up_round = (expert_up * norm_gain).astype(jnp.bfloat16)
    down_round = expert_down.astype(jnp.bfloat16)
    shared_gate_round = (shared_gate * norm_gain).astype(jnp.bfloat16)
    shared_up_round = (shared_up * norm_gain).astype(jnp.bfloat16)
    shared_down_round = shared_down.astype(jnp.bfloat16)
    tok_float = tokens.astype(jnp.float32)
    normed = (tok_float * lax.rsqrt(lax.optimization_barrier(jnp.mean(tok_float * tok_float, axis=1, keepdims=True)) + norm_eps)).astype(jnp.bfloat16)
    share = route_weight / lax.optimization_barrier(jnp.sum(route_weight, axis=1, keepdims=True)) * route_scale
    shared_act = feed_forward(normed, shared_gate_round, shared_up_round)
    shared_out = jnp.dot(shared_act, shared_down_round, preferred_element_type=jnp.float32)
    most_rows = EXPERTS * CAP

    def per_expert(total, expert):
        named = expert_ids == expert
        chosen = lax.optimization_barrier(jnp.sum(jnp.where(named, share, jnp.float32(0.0)), axis=1))
        present = jnp.any(named, axis=1)
        index = jnp.nonzero(present, size=most_rows, fill_value=0)[0].astype(jnp.int32)
        live = jnp.arange(most_rows).astype(jnp.int32) < jnp.sum(present.astype(jnp.int32))
        picked = normed[index]
        act = feed_forward(picked, gate_round[expert], up_round[expert])
        out = jnp.dot(act, down_round[expert], preferred_element_type=jnp.float32).astype(jnp.bfloat16)
        scale = jnp.where(live, chosen[index], jnp.float32(0.0))
        return (total.at[index].add(scale[:, None] * out.astype(jnp.float32)), None)
    start_total = jnp.zeros((TOKENS, D), jnp.float32)
    routed, _ = lax.scan(per_expert, start_total, jnp.arange(EXPERTS).astype(jnp.int32))
    mixed = (shared_out + routed).astype(jnp.bfloat16)
    new_gate = gate_round.reshape(N_GR, N_FS, FF, D)
    new_up = up_round.reshape(N_GR, N_FS, FF, D)
    new_down = down_round.reshape(N_GR, N_FS, FF, D)
    return (mixed, new_gate, new_up, new_down, shared_gate_round, shared_up_round, shared_down_round)
```

```python
import functools
import jax
import jax.numpy as jnp
from jax import lax
from jax.experimental import pallas as pl
from jax.experimental.pallas import tpu as pltpu
from jax.sharding import PartitionSpec as P

route_scale = 2.5
norm_eps = 1e-06


def fold_gain(weight, gain):
    return (weight * gain).astype(jnp.bfloat16)


def body(
    tokens,
    expert_ids,
    route_weight,
    norm_gain,
    expert_gate,
    expert_up,
    expert_down,
    shared_gate,
    shared_up,
    shared_down,
):
    group_count = lax.axis_size("gr")
    shard_count = lax.axis_size("fs")
    column_count = lax.axis_size("tp")
    tok_rows = tokens.shape[0]
    col_width = expert_gate.shape[2]
    top_count = expert_ids.shape[1]
    hidden = expert_gate.shape[1] * shard_count
    shared_hidden = shared_gate.shape[0] * shard_count
    experts = group_count * shard_count
    capacity = tok_rows * top_count * 5 // (4 * experts)
    gate_round = fold_gain(expert_gate, norm_gain)
    up_round = fold_gain(expert_up, norm_gain)
    down_round = expert_down.astype(jnp.bfloat16)
    moved = (
        lax.all_to_all(gate_round, "fs", split_axis=0, concat_axis=1, tiled=True),
        lax.all_to_all(up_round, "fs", split_axis=0, concat_axis=1, tiled=True),
        lax.all_to_all(down_round, "fs", split_axis=0, concat_axis=1, tiled=True),
    )
    whole = (
        lax.all_gather(moved[0], "gr", axis=0, tiled=True),
        lax.all_gather(moved[1], "gr", axis=0, tiled=True),
        lax.all_gather(moved[2], "gr", axis=0, tiled=True),
    )
    new_gate, new_up, new_down = tuple(
        (matrix.reshape(group_count, 1, hidden, col_width) for matrix in whole)
    )
    new_shared_gate, new_shared_up, new_shared_down = (
        lax.all_gather(fold_gain(shared_gate, norm_gain), "fs", axis=0, tiled=True),
        lax.all_gather(fold_gain(shared_up, norm_gain), "fs", axis=0, tiled=True),
        lax.all_gather(shared_down.astype(jnp.bfloat16), "fs", axis=0, tiled=True),
    )
    tok_float = tokens.astype(jnp.float32)
    normed = (
        tok_float * lax.rsqrt(jnp.mean(tok_float * tok_float, axis=1, keepdims=True) + norm_eps)
    ).astype(jnp.bfloat16)
    normed_cols = lax.dynamic_slice_in_dim(normed, lax.axis_index("tp") * col_width, col_width, 1)
    flat_expert = expert_ids.reshape(-1)
    one_hot = (flat_expert[:, None] == jnp.arange(experts, dtype=jnp.int32)[None, :]).astype(
        jnp.int32
    )
    running = jnp.cumsum(one_hot, axis=0)
    rank = jnp.sum((running - one_hot) * one_hot, axis=1)
    dest = flat_expert * capacity + rank
    token_of = jnp.arange(tok_rows * top_count, dtype=jnp.int32) // top_count
    slot_token = jnp.full((experts * capacity,), tok_rows, jnp.int32).at[dest].set(token_of)
    padded = jnp.concatenate([normed_cols, jnp.zeros((1, col_width), jnp.bfloat16)], axis=0)
    outgoing = padded[slot_token].reshape(group_count, shard_count, capacity, col_width)
    arrived = lax.all_to_all(outgoing, "fs", split_axis=1, concat_axis=1, tiled=True)
    slot_rows = arrived.reshape(group_count, shard_count * capacity, col_width)
    pair_weight = jnp.stack([new_gate[:, 0], new_up[:, 0]], axis=2).reshape(
        group_count, 2 * hidden, col_width
    )
    rows_weight = pair_weight
    term = jnp.einsum("ihd,ird->hir", rows_weight, slot_rows, preferred_element_type=jnp.float32)
    pair_sum = lax.psum_scatter(
        term.reshape(
            2 * hidden // column_count * lax.axis_size("tp"), group_count * shard_count * capacity
        ).astype(jnp.bfloat16),
        "tp",
        scatter_dimension=0,
        tiled=True,
    ).astype(jnp.float32)
    pair_sum = pair_sum.reshape(hidden // column_count, 2, group_count, shard_count * capacity)
    activation = (jax.nn.silu(pair_sum[:, 0]) * pair_sum[:, 1]).astype(jnp.bfloat16)
    down_local = new_down[:, 0]
    rows_down = down_local
    slot_out = jnp.einsum(
        "hir,ihd->ird",
        lax.all_gather(activation, "tp", axis=0, tiled=True),
        rows_down,
        preferred_element_type=jnp.float32,
    )
    returning = slot_out.astype(jnp.bfloat16).reshape(group_count, shard_count, capacity, col_width)
    returned = lax.all_to_all(returning, "fs", split_axis=1, concat_axis=1, tiled=True)
    result_rows = returned.reshape(experts * capacity, col_width)
    picked = result_rows[dest].reshape(tok_rows, top_count, col_width).astype(jnp.float32)
    share = route_weight / jnp.sum(route_weight, axis=1, keepdims=True) * route_scale
    routed = jnp.sum(share[:, :, None] * picked, axis=1)
    shared_pair = jnp.stack([new_shared_gate, new_shared_up], axis=1).reshape(
        2 * shared_hidden, col_width
    )
    rows_weight = shared_pair
    shared_sum = lax.psum_scatter(
        lax.dot_general(
            rows_weight, normed_cols, (((1,), (1,)), ((), ())), preferred_element_type=jnp.float32
        ).astype(jnp.bfloat16),
        "tp",
        scatter_dimension=0,
        tiled=True,
    ).astype(jnp.float32)
    shared_sum = shared_sum.reshape(shared_hidden // column_count, 2, tok_rows)
    shared_act = (jax.nn.silu(shared_sum[:, 0]) * shared_sum[:, 1]).astype(jnp.bfloat16)
    rows_down = new_shared_down
    shared_out = lax.dot_general(
        lax.all_gather(shared_act, "tp", axis=0, tiled=True),
        rows_down,
        (((0,), (0,)), ((), ())),
        preferred_element_type=jnp.float32,
    )
    mixed = (shared_out + routed).astype(jnp.bfloat16)
    return (mixed, new_gate, new_up, new_down, new_shared_gate, new_shared_up, new_shared_down)


def place_kernel(count, plan, offsets, *refs):
    sources, targets = refs[:count], refs[count:-3]
    room, in_sems, out_sems = refs[-3:]
    inward, outward, at = [], [], 0
    for number, (source, start, rows, target, slot, group) in enumerate(plan):
        row = pl.multiple_of(offsets[slot], rows)
        if group is None:
            where = targets[target].at[pl.ds(row, rows)]
        else:
            where = targets[target].at[offsets[group], 0, pl.ds(row, rows)]
        held = room.at[pl.ds(at, rows)]
        inward.append(
            pltpu.make_async_copy(sources[source].at[pl.ds(start, rows)], held, in_sems.at[number])
        )
        outward.append(pltpu.make_async_copy(held, where, out_sems.at[number]))
        at += rows
    for copy in inward:
        copy.start()
    for arriving, leaving in zip(inward, outward):
        arriving.wait()
        leaving.start()
    for copy in outward:
        copy.wait()


def place(offsets, sources, plan, shapes):
    anywhere = pl.BlockSpec(memory_space=pl.ANY)
    total = sum(entry[2] for entry in plan)
    return pl.pallas_call(
        functools.partial(place_kernel, len(sources), plan),
        out_shape=[jax.ShapeDtypeStruct(shape, jnp.bfloat16) for shape in shapes],
        in_specs=[pl.BlockSpec(memory_space=pltpu.SMEM)] + [anywhere] * len(sources),
        out_specs=[anywhere] * len(shapes),
        scratch_shapes=[
            pltpu.VMEM((total, shapes[0][-1]), jnp.bfloat16),
            pltpu.SemaphoreType.DMA((len(plan),)),
            pltpu.SemaphoreType.DMA((len(plan),)),
        ],
    )(offsets, *sources)


def pair_body(
    tokens,
    expert_ids,
    route_weight,
    norm_gain,
    expert_gate,
    expert_up,
    expert_down,
    shared_gate,
    shared_up,
    shared_down,
):
    n = lax.axis_size("fs")
    group, own, core = lax.axis_index("gr"), lax.axis_index("fs"), lax.axis_index("tp")
    tok_rows = tokens.shape[0]
    part = expert_gate.shape[1]
    width = expert_gate.shape[2]
    hidden = part * n
    experts = lax.axis_size("gr") * n
    half = part // 2
    swap = [(0, 1), (1, 0)]
    cycle = list(range(0, n, 2)) + list(range(n - 1, 0, -2))
    ahead = [(cycle[i], cycle[(i + 1) % n]) for i in range(n)]
    back = [(b, a) for a, b in ahead]

    tok_float = tokens.astype(jnp.float32)
    scale = lax.rsqrt(jnp.mean(tok_float * tok_float, axis=1, keepdims=True) + norm_eps)
    normed = (
        lax.dynamic_slice_in_dim(tokens, core * width, width, 1).astype(jnp.float32) * scale
    ).astype(jnp.bfloat16)
    share = route_weight / jnp.sum(route_weight, axis=1, keepdims=True) * route_scale
    named = expert_ids[:, :, None] == jnp.arange(experts, dtype=jnp.int32)[None, None, :]
    share_of = jnp.sum(jnp.where(named, share[:, :, None], 0.0), axis=1)

    def ring(block):
        near, far = {0: block}, block
        for step in range(1, n // 2 + 1):
            far = lax.ppermute(far, "fs", ahead)
            near[-step] = far
        far = block
        for step in range(1, (n - 1) // 2 + 1):
            far = lax.ppermute(far, "fs", back)
            near[step] = far
        return near

    rel = list(range(-(n // 2), (n - 1) // 2 + 1))
    rows_of = ring(normed)
    shares_of = ring(share_of)

    def pieces(slot):
        to = own ^ slot ^ core
        pick = lambda a: lax.dynamic_index_in_dim(a, to, 0, keepdims=False)
        pair = jnp.concatenate(
            [fold_gain(pick(expert_gate), norm_gain), fold_gain(pick(expert_up), norm_gain)], 0
        )
        return pair, pick(expert_down).astype(jnp.bfloat16)

    def hop(slot):
        return [(2 * f + t, 2 * (f ^ slot ^ t) + t) for f in range(n) for t in range(2)]

    order = sorted(range(n), reverse=True)
    sent = {slot: pieces(slot) for slot in order}
    pair_in = {slot: lax.ppermute(sent[slot][0], ("fs", "tp"), hop(slot)) for slot in order}
    down_in = {slot: lax.ppermute(sent[slot][1], ("fs", "tp"), hop(slot)) for slot in order}
    pair_out = {slot: lax.ppermute(pair_in[slot], "gr", swap) for slot in order[::-1]}
    down_out = {slot: lax.ppermute(down_in[slot], "gr", swap) for slot in order[::-1]}

    shared_pair = (fold_gain(shared_gate, norm_gain), fold_gain(shared_up, norm_gain))
    shared_low = shared_down.astype(jnp.bfloat16)
    shared_of = ring(jnp.concatenate([*shared_pair, shared_low], 0))

    def cut(a, side):
        return lax.dynamic_slice_in_dim(a, side * half, half, 0)

    def up_rows(parity, side):
        slots = range(parity, n, 2)
        rows = [held[s][i * part : (i + 1) * part] for i in range(2) for held in (pair_in, pair_out) for s in slots]
        return jnp.concatenate(rows + [cut(a, side) for a in shared_pair], 0)

    def down_rows(parity, side):
        slots = range(parity, n, 2)
        rows = [held[s] for held in (down_in, down_out) for s in slots]
        return jnp.concatenate(rows + [cut(shared_low, side)], 0)

    rows = jnp.concatenate([rows_of[r] for r in rel], 0)
    contract = (((1,), (1,)), ((), ()))
    theirs = lax.dot_general(rows, up_rows(1, 1 - core), contract, preferred_element_type=jnp.float32)
    arrived = lax.ppermute(theirs.astype(jnp.bfloat16), "tp", swap)
    mine = lax.dot_general(rows, up_rows(0, core), contract, preferred_element_type=jnp.float32)
    pre = mine + arrived.astype(jnp.float32)
    share_all = jnp.concatenate([shares_of[r] for r in rel], 0)
    index = jnp.arange(experts)
    factors = [
        jnp.sum(jnp.where(index == side * n + own, share_all, 0.0), axis=1, keepdims=True)
        for side in (group, 1 - group)
    ]
    factor = jnp.concatenate(
        [jnp.broadcast_to(f, (rows.shape[0], hidden // 2)) for f in factors], 1
    )
    act = (jax.nn.silu(pre[:, :hidden]) * pre[:, hidden : 2 * hidden] * factor).astype(jnp.bfloat16)
    shared_act = (
        jax.nn.silu(pre[:, 2 * hidden : 2 * hidden + half]) * pre[:, 2 * hidden + half :]
    ).astype(jnp.bfloat16)
    act_mine = jnp.concatenate([act, shared_act], 1)
    act_theirs = lax.ppermute(act_mine, "tp", swap)
    down_mine, down_theirs = down_rows(0, core), down_rows(1, 1 - core)

    def out_of(r):
        at = slice(rel.index(r) * tok_rows, (rel.index(r) + 1) * tok_rows)
        return jnp.dot(act_mine[at], down_mine, preferred_element_type=jnp.float32) + jnp.dot(
            act_theirs[at], down_theirs, preferred_element_type=jnp.float32
        )

    total = out_of(0)
    for sign, perm, steps in ((-1, back, n // 2), (1, ahead, (n - 1) // 2)):
        moving = None
        for step in range(steps, 0, -1):
            value = out_of(sign * step)
            if moving is not None:
                value = value + moving.astype(jnp.float32)
            moving = lax.ppermute(value.astype(jnp.bfloat16), "fs", perm)
        total = total + moving.astype(jnp.float32)
    mixed = total.astype(jnp.bfloat16)

    slots = list(range(n))
    offsets = jnp.stack([(own ^ s ^ core) * part for s in slots] + [group, 1 - group]).astype(jnp.int32)
    sources, plan = [], []
    for at, (pairs, lows) in ((n, (pair_in, down_in)), (n + 1, (pair_out, down_out))):
        for s in slots:
            plan.append((len(sources), 0, part, 0, s, at))
            plan.append((len(sources), part, part, 1, s, at))
            sources.append(pairs[s])
            plan.append((len(sources), 0, part, 2, s, at))
            sources.append(lows[s])
    shape = (lax.axis_size("gr"), 1, hidden, width)
    new_gate, new_up, new_down = place(offsets, sources, plan, [shape] * 3)

    table = jnp.array(cycle, jnp.int32)
    spot = jnp.sum(jnp.where(table == own, jnp.arange(n, dtype=jnp.int32), 0))
    from_of = jnp.stack(
        [jnp.sum(jnp.where(jnp.arange(n) == (spot + r) % n, table, 0)) * part for r in rel]
    ).astype(jnp.int32)
    plan = [(i, k * part, part, k, i, None) for i in range(n) for k in range(3)]
    new_shared = place(from_of, [shared_of[r] for r in rel], plan, [(hidden, width)] * 3)
    return (mixed, new_gate, new_up, new_down, *new_shared)


def solution(mesh):
    size = dict(mesh.shape)
    paired = size["gr"] == 2 and size["tp"] == 2 and size["fs"] & (size["fs"] - 1) == 0
    placed = (
        P(("gr", "fs"), None),
        P(("gr", "fs"), None),
        P(("gr", "fs"), None),
        P("tp"),
        P("gr", "fs", "tp"),
        P("gr", "fs", "tp"),
        P("gr", "fs", "tp"),
        P("fs", "tp"),
        P("fs", "tp"),
        P("fs", "tp"),
    )
    return jax.shard_map(
        pair_body if paired else body,
        mesh=mesh,
        in_specs=placed,
        out_specs=(
            P(("gr", "fs"), "tp"),
            P(None, "fs", None, "tp"),
            P(None, "fs", None, "tp"),
            P(None, "fs", None, "tp"),
            P(None, "tp"),
            P(None, "tp"),
            P(None, "tp"),
        ),
        check_vma=False,
    )
```
